32 devices in a mesh: ep: 32 (over z, y, x, core).
Axes of the slice: x: 2, y: 2, z: 4, core: 2. Of those that a mesh axis runs over, the one named last changes fastest.
Arguments:
- residual: bfloat16 [2048, 2048], P('ep'), may hold values from -6 to 6
- branch_in: bfloat16 [2048, 1024], P('ep'), may hold values from -6 to 6
- state_real: float32 [2048, 4096], P('ep'), may hold values from -4 to 4
- state_imag: float32 [2048, 4096], P('ep'), may hold values from -4 to 4
- decay_rate: float32 [64, 64], replicated, may hold values from 0.1 to 1
- frequency: float32 [64, 64], replicated, may hold values from 0 to 200
- log_step: float32 [64], replicated, may hold values from -4 to 0
- input_real: bfloat16 [64, 64, 16], replicated, may hold values from -1 to 1
- input_imag: bfloat16 [64, 64, 16], replicated, may hold values from -1 to 1
- output_matrix_real: bfloat16 [64, 16, 64], replicated, may hold values from -0.5 to 0.5
- output_matrix_imaginary: bfloat16 [64, 16, 64], replicated, may hold values from -0.5 to 0.5
- skip_gain: float32 [1024], replicated, may hold values from -4 to 4
- glu_value: bfloat16 [1024, 2048], replicated, may hold values from -0.1875 to 0.1875
- glu_gate: bfloat16 [1024, 2048], replicated, may hold values from -0.1875 to 0.1875
- mix_gain: float32 [2048], replicated, may hold values from 0.1 to 1.9
- moe_in_gain: float32 [2048], replicated, may hold values from 0.1 to 1.9
- moe_out_gain: float32 [2048], replicated, may hold values from 0.1 to 1.9
- routes: int32 [2048, 6], P('ep'), may hold values from 0 to 31, all different within a row; in each aligned block of 64 rows (0 to 63, 64 to 127, ...) at most 16 rows name the same one
- route_weights: float32 [2048, 6], P('ep'), may hold values from 0.05 to 0.6
- expert_gate: bfloat16 [32, 2048, 512], P('ep'), may hold values from -0.125 to 0.125
- expert_up: bfloat16 [32, 2048, 512], P('ep'), may hold values from -0.125 to 0.125
- expert_down: bfloat16 [32, 512, 2048], P('ep'), may hold values from -0.25 to 0.25
- shared_gate: bfloat16 [2048, 512], replicated, may hold values from -0.125 to 0.125
- shared_up: bfloat16 [2048, 512], replicated, may hold values from -0.125 to 0.125
- shared_down: bfloat16 [512, 2048], replicated, may hold values from -0.25 to 0.25
Outputs:
- layer_out: bfloat16 [2048, 2048], P('ep')
- next_real: float32 [2048, 4096], P('ep')
- next_imag: float32 [2048, 4096], P('ep')
The draws below stay inside these ranges and needn't reach their ends.
Inputs may be any that keep to these rules, and one draw needn't show every extreme that they name: `routes`: among the rows of one device no expert is named more than 16 times, and in every draw some expert is named exactly 16 times by some device's rows; a token's experts are distinct.
All inputs are finite; a program needn't handle non-finite values.
Results may differ from the reference program's by a relative error of at most 0.0066.
Values may be sent and summed in bfloat16 or wider, within the bound.
A program may use at most 128 MiB of HBM per device.

```python
import math
import jax
import jax.numpy as jnp
import numpy as np
from jax import lax

D = 2048
SSM_W = 1024
GCH = 16
GROUPS = 64
STATE = 64
EH = 512
TOP_K = 6
SEQ_DEV = 64
SEQS = 2048
EXPERTS = 32
CAP = 16
N_EP = 32


def levels(key, shape, pieces, least, largest):
    def one(dim, shards_of):
        steps = jax.random.uniform(jax.random.fold_in(jax.random.fold_in(key, 6), dim), (shards_of,), jnp.float32, least / len(pieces), largest / len(pieces))
        return jnp.repeat(jnp.exp(steps), shape[dim] // shards_of).reshape((-1,) + (1,) * (len(shape) - dim - 1))

    factor_of = one(*pieces[0])
    for cut in pieces[1:]:
        factor_of = factor_of * one(*cut)
    return factor_of


def shared_out(key, own, number, rows, amount, top, most, lean):
    ranking = jax.random.permutation(key, amount)
    heavy_load, ordinary = portions_of(amount, rows * top, most, lean, True), portions_of(amount, rows * top, most, lean, False)
    places = jnp.arange(amount)

    def named(sizes, rotation):
        used = int((sizes > 0).sum())
        fixed = max(1, used // 4)
        moved = fixed + (places - fixed + rotation * (used - fixed)) % max(1, amount - fixed)
        return jnp.zeros((amount,), jnp.int32).at[ranking[jnp.where(places < fixed, places, moved)]].set(jnp.asarray(sizes, jnp.int32))

    sizes = jnp.where(number % 4 == 0, named(heavy_load, number // 4), named(ordinary, number - number // 4 - 1))
    mixed = jax.random.permutation(jax.random.fold_in(own, 3), amount)
    source_of, sink = mixed[0:amount // 2 * 2:2], mixed[1:amount // 2 * 2:2]
    slack = jnp.minimum(sizes[source_of] - 1, most - sizes[sink]) // 2
    slack = jnp.where((source_of == ranking[0]) | (sink == ranking[0]) | (sizes[sink] == 0), 0, jnp.maximum(slack, 0))
    moved = jax.random.randint(jax.random.fold_in(own, 4), (amount // 2,), 0, 1 << 20) % (slack + 1)
    sizes = sizes.at[source_of].add(-moved).at[sink].add(moved)
    items = jnp.searchsorted(jnp.cumsum(sizes), jnp.arange(rows * top), side="right").astype(jnp.int32)
    table = items.reshape(top, rows).T
    table = table[jax.random.permutation(jax.random.fold_in(own, 1), rows)]
    rotation = jax.random.randint(jax.random.fold_in(own, 2), (rows, 1), 0, top)
    return jnp.take_along_axis(table, (jnp.arange(top)[None, :] + rotation) % top, axis=1)


def portions_of(amount, total, reach, skew, full):
    weights = [(1 << 20) // math.isqrt(rank ** skew) + 1 for rank in range(1, amount + 1)]
    largest = reach if full else min(reach, max(-(-total // amount), total * weights[0] // sum(weights)))
    least = 1 if total - largest >= amount - 1 else 0
    given, surplus = [largest] + [least] * (amount - 1), total - largest - least * (amount - 1)
    while surplus > 0:
        candidates = [i for i in range(1, amount) if given[i] < largest] or [i for i in range(1, amount) if given[i] < reach]
        whole, left = sum([weights[i] for i in candidates]), surplus
        for i in candidates:
            more = min(reach - given[i], max(1, left * weights[i] // whole), surplus)
            given[i] = given[i] + more
            surplus = surplus - more
    return np.array(given)


def bell_draw(rng, shape, deviation, reach, split=(), kind=jnp.bfloat16):
    loudness = levels(rng, shape, split, -0.22, 0.18) if split else 1.0
    array = jax.random.normal(rng, shape, jnp.float32) * deviation * loudness
    return jnp.minimum(jnp.maximum(array, -reach), reach).astype(kind)


def setup_inputs(seed: int = 0) -> dict:
    arg_keys = jax.random.split(jax.random.key(seed), 26)
    residual = bell_draw(arg_keys[0], (SEQS, D), 1.0, 6.0, ((0, 32),))
    branch_in = bell_draw(arg_keys[1], (SEQS, SSM_W), 1.0, 6.0, ((0, 32),))
    state_real = bell_draw(arg_keys[2], (SEQS, GROUPS * STATE), 0.5, 4.0, ((0, 32),), jnp.float32)
    state_imag = bell_draw(arg_keys[3], (SEQS, GROUPS * STATE), 0.5, 4.0, ((0, 32),), jnp.float32)
    decay_rate = jnp.clip(jnp.exp(jax.random.uniform(arg_keys[4], (GROUPS, STATE), jnp.float32, math.log(0.1), math.log(1.0))), 0.1, 1.0)
    frequency = jnp.clip(jax.random.uniform(arg_keys[5], (GROUPS, STATE), jnp.float32, 0.0, 200.0), 0.0, 200.0)
    log_step = jnp.clip(jax.random.uniform(arg_keys[6], (GROUPS,), jnp.float32, -4.0, 0.0), -4.0, 0.0)
    input_real = bell_draw(arg_keys[7], (GROUPS, STATE, GCH), (2 * GCH) ** -0.5, 1.0)
    input_imag = bell_draw(arg_keys[8], (GROUPS, STATE, GCH), (2 * GCH) ** -0.5, 1.0)
    output_matrix_real = bell_draw(arg_keys[9], (GROUPS, GCH, STATE), (2 * STATE) ** -0.5, 0.5)
    output_matrix_imaginary = bell_draw(arg_keys[10], (GROUPS, GCH, STATE), (2 * STATE) ** -0.5, 0.5)
    skip_gain = bell_draw(arg_keys[11], (SSM_W,), 1.0, 4.0, (), jnp.float32)
    glu_value = bell_draw(arg_keys[12], (SSM_W, D), SSM_W ** -0.5, 0.1875)
    glu_gate = bell_draw(arg_keys[13], (SSM_W, D), SSM_W ** -0.5, 0.1875)
    mix_gain = jnp.clip(1.0 + 0.18 * jax.random.normal(arg_keys[14], (D,), jnp.float32), 0.1, 1.9)
    moe_in_gain = jnp.clip(1.0 + 0.18 * jax.random.normal(arg_keys[15], (D,), jnp.float32), 0.1, 1.9)
    moe_out_gain = jnp.clip(1.0 + 0.18 * jax.random.normal(arg_keys[16], (D,), jnp.float32), 0.1, 1.9)
    routes_keys = jax.random.split(jax.random.fold_in(arg_keys[17], 1), SEQS // SEQ_DEV)
    routes_turns = jax.random.permutation(jax.random.fold_in(arg_keys[17], 3), SEQS // SEQ_DEV)
    routes = jax.vmap(lambda own, number: shared_out(jax.random.fold_in(arg_keys[17], 2), own, number, SEQ_DEV, EXPERTS, TOP_K, CAP, 2))(routes_keys, routes_turns).reshape((SEQS, TOP_K))
    route_weights = jnp.clip(0.05 + 0.55 * jax.random.uniform(arg_keys[18], (SEQS, TOP_K), jnp.float32) ** levels(arg_keys[18], (SEQS, TOP_K), ((0, 32),), -0.2, 0.2), 0.05, 0.6)
    expert_gate = bell_draw(arg_keys[19], (EXPERTS, D, EH), D ** -0.5, 0.125, ((0, 32),))
    expert_up = bell_draw(arg_keys[20], (EXPERTS, D, EH), D ** -0.5, 0.125, ((0, 32),))
    expert_down = bell_draw(arg_keys[21], (EXPERTS, EH, D), EH ** -0.5, 0.25, ((0, 32),))
    shared_gate = bell_draw(arg_keys[22], (D, EH), D ** -0.5, 0.125)
    shared_up = bell_draw(arg_keys[23], (D, EH), D ** -0.5, 0.125)
    shared_down = bell_draw(arg_keys[24], (EH, D), EH ** -0.5, 0.25)
    return dict(residual=residual, branch_in=branch_in, state_real=state_real, state_imag=state_imag, decay_rate=decay_rate, frequency=frequency, log_step=log_step, input_real=input_real, input_imag=input_imag, output_matrix_real=output_matrix_real, output_matrix_imaginary=output_matrix_imaginary, skip_gain=skip_gain, glu_value=glu_value, glu_gate=glu_gate, mix_gain=mix_gain, moe_in_gain=moe_in_gain, moe_out_gain=moe_out_gain, routes=routes, route_weights=route_weights, expert_gate=expert_gate, expert_up=expert_up, expert_down=expert_down, shared_gate=shared_gate, shared_up=shared_up, shared_down=shared_down)


norm_eps = 1e-06

def scaled_norm(row_block, norm_gain):
    return row_block * lax.rsqrt(lax.optimization_barrier(jnp.mean(row_block * row_block, axis=-1, keepdims=True)) + norm_eps) * norm_gain

def state_step(branch_in, state_real, state_imag, decay_rate, frequency, log_step, input_real, input_imag, output_matrix_real, output_matrix_imaginary, skip_gain):
    seq_count = branch_in.shape[0]
    group_count, state_count = decay_rate.shape
    chan_count = input_real.shape[2]
    step_size = jnp.exp(log_step)[:, None]
    magnitude = jnp.exp(-decay_rate * step_size)
    abar_re = magnitude * jnp.cos(frequency * step_size)
    abar_im = magnitude * jnp.sin(frequency * step_size)
    lam_re = -decay_rate
    lam_im = frequency
    denominator = lam_re * lam_re + lam_im * lam_im
    numer_re = abar_re - 1.0
    coef_re = (numer_re * lam_re + abar_im * lam_im) / denominator
    coef_im = (abar_im * lam_re - numer_re * lam_im) / denominator
    b_real = input_real.astype(jnp.float32)
    b_imag = input_imag.astype(jnp.float32)
    bbar_re = coef_re[..., None] * b_real - coef_im[..., None] * b_imag
    bbar_im = coef_re[..., None] * b_imag + coef_im[..., None] * b_real
    feed_rows = branch_in.astype(jnp.float32).reshape(seq_count, group_count, chan_count)
    forcing_real = jnp.einsum('tgc,gpc->tgp', feed_rows, bbar_re, precision=lax.Precision.HIGHEST)
    drive_im = jnp.einsum('tgc,gpc->tgp', feed_rows, bbar_im, precision=lax.Precision.HIGHEST)
    old_re = state_real.reshape(seq_count, group_count, state_count)
    old_im = state_imag.reshape(seq_count, group_count, state_count)
    fresh_real = abar_re * old_re - abar_im * old_im + forcing_real
    fresh_imaginary = abar_re * old_im + abar_im * old_re + drive_im
    state_readout = jnp.einsum('ukb,krb->ukr', fresh_real, output_matrix_real.astype(jnp.float32), precision=lax.Precision.HIGHEST) - jnp.einsum('ukb,krb->ukr', fresh_imaginary, output_matrix_imaginary.astype(jnp.float32), precision=lax.Precision.HIGHEST)
    mixed_rows = state_readout.reshape(seq_count, group_count * chan_count) + skip_gain * branch_in.astype(jnp.float32)
    activated = jax.nn.gelu(mixed_rows).astype(jnp.bfloat16)
    return (activated, fresh_real.reshape(seq_count, -1), fresh_imaginary.reshape(seq_count, -1))

def expert_rows(row_block, w_gate, w_up, w_down):
    gate_part = jnp.dot(row_block, w_gate, preferred_element_type=jnp.float32)
    up_part = jnp.dot(row_block, w_up, preferred_element_type=jnp.float32)
    hidden = (jax.nn.silu(gate_part) * up_part).astype(jnp.bfloat16)
    return jnp.dot(hidden, w_down, preferred_element_type=jnp.float32)

def mixer_residual(residual, activated, glu_value, glu_gate, mix_gain):
    value_part = jnp.dot(activated, glu_value, preferred_element_type=jnp.float32)
    gate_part = jnp.dot(activated, glu_gate, preferred_element_type=jnp.float32)
    branch = value_part * jax.nn.sigmoid(gate_part)
    return (residual.astype(jnp.float32) + scaled_norm(branch, mix_gain)).astype(jnp.bfloat16)

def reference(residual, branch_in, state_real, state_imag, decay_rate, frequency, log_step, input_real, input_imag, output_matrix_real, output_matrix_imaginary, skip_gain, glu_value, glu_gate, mix_gain, moe_in_gain, moe_out_gain, routes, route_weights, expert_gate, expert_up, expert_down, shared_gate, shared_up, shared_down):
    activated, next_real, next_imag = state_step(branch_in, state_real, state_imag, decay_rate, frequency, log_step, input_real, input_imag, output_matrix_real, output_matrix_imaginary, skip_gain)
    resid_mid = mixer_residual(residual, activated, glu_value, glu_gate, mix_gain)
    normed = scaled_norm(resid_mid.astype(jnp.float32), moe_in_gain).astype(jnp.bfloat16)
    hidden_width = normed.shape[1]
    flat_routes = routes.reshape(-1).astype(jnp.int32)
    assign_count = flat_routes.shape[0]
    sorted_order = jnp.argsort(flat_routes, stable=True).astype(jnp.int32)
    sorted_expert = flat_routes[sorted_order]
    expert_load = lax.optimization_barrier(jnp.sum((flat_routes[:, None] == jnp.arange(EXPERTS, dtype=jnp.int32)[None, :]).astype(jnp.int32), axis=0))
    load_start = jnp.cumsum(expert_load) - expert_load
    slot_rank = jnp.arange(assign_count, dtype=jnp.int32) - load_start[sorted_expert]
    slot_most = CAP * N_EP
    slot_index = (sorted_expert * slot_most + slot_rank).astype(jnp.int32)
    slot_table = jnp.full((EXPERTS * slot_most,), SEQS, jnp.int32).at[slot_index].set(sorted_order // TOP_K)
    padded = jnp.concatenate([normed, jnp.zeros((1, hidden_width), jnp.bfloat16)], axis=0)

    def one_expert(expert_args):
        row_ids, w_gate, w_up, w_down = expert_args
        return expert_rows(padded[row_ids], w_gate, w_up, w_down).astype(jnp.bfloat16)
    expert_out = lax.map(one_expert, (slot_table.reshape(EXPERTS, slot_most), expert_gate, expert_up, expert_down))
    assign_slot = jnp.zeros((assign_count,), jnp.int32).at[sorted_order].set(slot_index)
    per_assign = expert_out.reshape(-1, hidden_width)[assign_slot].reshape(SEQS, TOP_K, hidden_width).astype(jnp.float32)
    routed = lax.optimization_barrier(jnp.sum(per_assign * route_weights[..., None], axis=1))
    shared = expert_rows(normed, shared_gate, shared_up, shared_down)
    combined = shared + routed
    layer_out = (resid_mid.astype(jnp.float32) + scaled_norm(combined, moe_out_gain)).astype(jnp.bfloat16)
    return (layer_out, next_real, next_imag)
```

```python
import functools

import jax
import jax.numpy as jnp
from jax import lax
from jax.experimental import pallas as pl
from jax.experimental.pallas import tpu as pltpu
from jax.sharding import PartitionSpec as P

norm_eps = 1e-06
ROW_TILE = 16
MESH = pl.DeviceIdType.MESH


def scaled_norm(row_block, norm_gain):
    return (
        row_block
        * lax.rsqrt(jnp.mean(row_block * row_block, axis=-1, keepdims=True) + norm_eps)
        * norm_gain
    )


def flipped(index, mask):
    out, bit = 0, 1
    while bit <= mask or bit == 1:
        digit = (index // bit) % 2
        out = out + bit * ((digit + 1) % 2 if mask & bit else digit)
        bit *= 2
    return out + (index // bit) * bit


def moe_kernel(
    planes,
    width,
    cap,
    normed,
    resid,
    slot_weights,
    out_gain,
    eg_hbm,
    eu_hbm,
    ed_hbm,
    sg_hbm,
    su_hbm,
    sd_hbm,
    out,
    eg,
    eu,
    ed,
    sg,
    su,
    sd,
    col_rows,
    col_weights,
    x_send,
    x_recv,
    y_send,
    y_recv,
    p_send,
    p_recv,
    total,
    load_sem,
    own_sem,
    row_s,
    row_r,
    wt_s,
    wt_r,
    x_s,
    x_r,
    y_s,
    y_r,
    p_s,
    p_r,
):
    me = lax.axis_index("ep")
    z = me // width
    p = me % width
    model = normed.shape[1]
    chunk = min(512, model)
    loads = [
        pltpu.make_async_copy(src, dst, load_sem.at[i])
        for i, (src, dst) in enumerate(
            ((sg_hbm, sg), (su_hbm, su), (sd_hbm, sd), (eg_hbm, eg), (eu_hbm, eu), (ed_hbm, ed))
        )
    ]
    for load in loads:
        load.start()

    barrier = pltpu.get_barrier_semaphore()
    for d in range(1, planes):
        pl.semaphore_signal(
            barrier, inc=1, device_id=(flipped(z, d) * width + p,), device_id_type=MESH
        )
    for r in range(1, width):
        pl.semaphore_signal(
            barrier, inc=1, device_id=(z * width + flipped(p, r),), device_id_type=MESH
        )
    pl.semaphore_wait(barrier, planes - 1 + width - 1)

    sends = []

    def send(src, dst, send_sem, recv_sem, target):
        copy = pltpu.make_async_remote_copy(
            src_ref=src,
            dst_ref=dst,
            send_sem=send_sem,
            recv_sem=recv_sem,
            device_id=(target,),
            device_id_type=MESH,
        )
        copy.start()
        sends.append(copy)

    def part(buf, d, q):
        return buf.at[d, pl.ds(pl.multiple_of(q * cap, cap), cap)]

    for d in range(1, planes):
        zt = flipped(z, d)
        target = zt * width + p
        send(slot_weights.at[zt], col_weights.at[d], wt_s.at[d], wt_r.at[d], target)
        send(normed, col_rows.at[d], row_s.at[d], row_r.at[d], target)

    def arrive(buf, sem):
        pltpu.make_async_copy(buf, buf, sem).wait()

    def block_weights(d):
        return slot_weights[z] if d == 0 else col_weights[d]

    def exchange(src, dst, d, send_sems, recv_sems, own):
        for r in range(1, width):
            q = flipped(p, r)
            send(
                part(src, d, q),
                part(dst, d, p),
                send_sems.at[d, r],
                recv_sems.at[d, r],
                z * width + q,
            )
        own_copy = pltpu.make_async_copy(part(src, d, p), part(dst, d, p), own)
        own_copy.start()

    def gathered(src, dst, d, recv_sems, own):
        for r in range(1, width):
            arrive(part(dst, d, flipped(p, r)), recv_sems.at[d, r])
        pltpu.make_async_copy(part(src, d, p), part(dst, d, p), own).wait()

    def dispatch(d):
        if d:
            arrive(col_weights.at[d], wt_r.at[d])
            arrive(col_rows.at[d], row_r.at[d])
        picks = jnp.where(block_weights(d).T > 0.0, 1.0, 0.0).astype(jnp.bfloat16)
        for c in range(0, model, chunk):
            rows = normed[:, c : c + chunk] if d == 0 else col_rows[d, :, c : c + chunk]
            x_send[d, :, c : c + chunk] = jnp.dot(
                picks, rows, preferred_element_type=jnp.float32
            ).astype(jnp.bfloat16)
        exchange(x_send, x_recv, d, x_s, x_r, own_sem.at[0, d])

    def hidden(rows, w_gate, w_up):
        gate_part = jnp.dot(rows, w_gate[...], preferred_element_type=jnp.float32)
        up_part = jnp.dot(rows, w_up[...], preferred_element_type=jnp.float32)
        return (jax.nn.silu(gate_part) * up_part).astype(jnp.bfloat16)

    def expert(d):
        gathered(x_send, x_recv, d, x_r, own_sem.at[0, d])
        if d == 0:
            for load in loads[3:]:
                load.wait()
        mid = hidden(x_recv[d], eg, eu)
        for c in range(0, model, chunk):
            y_send[d, :, c : c + chunk] = jnp.dot(
                mid, ed[:, c : c + chunk], preferred_element_type=jnp.float32
            ).astype(jnp.bfloat16)
        exchange(y_send, y_recv, d, y_s, y_r, own_sem.at[1, d])

    def combine(d):
        gathered(y_send, y_recv, d, y_r, own_sem.at[1, d])
        weights = block_weights(d)
        high = weights.astype(jnp.bfloat16)
        low = (weights - high.astype(jnp.float32)).astype(jnp.bfloat16)
        for c in range(0, model, chunk):
            rows = y_recv[d, :, c : c + chunk]
            partial = jnp.dot(high, rows, preferred_element_type=jnp.float32) + jnp.dot(
                low, rows, preferred_element_type=jnp.float32
            )
            if d == 0:
                total[:, c : c + chunk] += partial
            else:
                p_send[d, :, c : c + chunk] = partial.astype(jnp.bfloat16)
        if d:
            send(
                p_send.at[d], p_recv.at[d], p_s.at[d], p_r.at[d], flipped(z, d) * width + p
            )

    dispatch(0)
    for load in loads[:3]:
        load.wait()
    mid = hidden(normed[...], sg, su)
    for c in range(0, model, chunk):
        total[:, c : c + chunk] = jnp.dot(
            mid, sd[:, c : c + chunk], preferred_element_type=jnp.float32
        )
    for step in range(1, planes + 2):
        if step < planes:
            dispatch(step)
        if step - 1 < planes:
            expert(step - 1)
        if step >= 2:
            combine(step - 2)
    for d in range(1, planes):
        arrive(p_recv.at[d], p_r.at[d])
    combined = total[...]
    for d in range(1, planes):
        combined = combined + p_recv[d].astype(jnp.float32)
    out[...] = (
        resid[...].astype(jnp.float32) + scaled_norm(combined, out_gain[...])
    ).astype(out.dtype)
    for copy in sends:
        copy.wait_send()


def moe_layer(
    normed, resid_mid, slot_weights, moe_out_gain, experts, shared_weights, planes, width, cap
):
    seq_count, model = normed.shape
    half = jnp.bfloat16
    vmem = pl.BlockSpec(memory_space=pltpu.VMEM)
    hbm = pl.BlockSpec(memory_space=pl.ANY)
    slots = (planes, width * cap, model)
    dense = (planes, seq_count, model)
    dma = pltpu.SemaphoreType.DMA
    weights = (*experts, *shared_weights)
    return pl.pallas_call(
        functools.partial(moe_kernel, planes, width, cap),
        out_shape=jax.ShapeDtypeStruct((seq_count, model), half),
        in_specs=[vmem] * 4 + [hbm] * 6,
        out_specs=vmem,
        scratch_shapes=[pltpu.VMEM(w.shape, w.dtype) for w in weights]
        + [
            pltpu.VMEM(dense, half),
            pltpu.VMEM(slot_weights.shape, jnp.float32),
            pltpu.VMEM(slots, half),
            pltpu.VMEM(slots, half),
            pltpu.VMEM(slots, half),
            pltpu.VMEM(slots, half),
            pltpu.VMEM(dense, half),
            pltpu.VMEM(dense, half),
            pltpu.VMEM((seq_count, model), jnp.float32),
            dma((6,)),
            dma((2, planes)),
            dma((planes,)),
            dma((planes,)),
            dma((planes,)),
            dma((planes,)),
            dma((planes, width)),
            dma((planes, width)),
            dma((planes, width)),
            dma((planes, width)),
            dma((planes,)),
            dma((planes,)),
        ],
        compiler_params=pltpu.CompilerParams(
            collective_id=0, has_side_effects=True, vmem_limit_bytes=60 * 1024 * 1024
        ),
        name="moe_exchange",
    )(normed, resid_mid, slot_weights, moe_out_gain[None, :], *weights)


def slot_table(routes, route_weights, planes, width, cap):
    seq_count, top_count = routes.shape
    columns = planes * width * cap
    column = jnp.arange(columns, dtype=jnp.int32)
    column_expert = (column // cap).reshape(planes, 1, width * cap)
    column_slot = (column % cap).reshape(planes, 1, width * cap)
    match = routes.T[:, None, :, None] == column_expert[None]
    chosen = jnp.any(match, axis=0)
    weight = jnp.sum(jnp.where(match, route_weights.T[:, None, :, None], 0.0), axis=0)
    earlier = jnp.tril(jnp.ones((seq_count, seq_count), jnp.bfloat16), -1)
    rank = jnp.einsum(
        "ut,ztj->zuj", earlier, chosen.astype(jnp.bfloat16), preferred_element_type=jnp.float32
    )
    return jnp.where(chosen & (rank == column_slot.astype(jnp.float32)), weight, 0.0)


def state_step(
    branch_in,
    state_real,
    state_imag,
    decay_rate,
    frequency,
    log_step,
    input_real,
    input_imag,
    output_matrix_real,
    output_matrix_imaginary,
    skip_gain,
):
    seq_count = branch_in.shape[0]
    group_count, state_count = decay_rate.shape
    chan_count = input_real.shape[2]
    step_size = jnp.exp(log_step)[:, None]
    magnitude = jnp.exp(-decay_rate * step_size)
    abar_re = magnitude * jnp.cos(frequency * step_size)
    abar_im = magnitude * jnp.sin(frequency * step_size)
    lam_re = -decay_rate
    denominator = lam_re * lam_re + frequency * frequency
    numer_re = abar_re - 1.0
    coef_re = (numer_re * lam_re + abar_im * frequency) / denominator
    coef_im = (abar_im * lam_re - numer_re * frequency) / denominator
    b_real = input_real.astype(jnp.float32)
    b_imag = input_imag.astype(jnp.float32)
    bbar_re = coef_re[..., None] * b_real - coef_im[..., None] * b_imag
    bbar_im = coef_re[..., None] * b_imag + coef_im[..., None] * b_real
    feed_rows = branch_in.astype(jnp.float32).reshape(seq_count, group_count, chan_count)
    forcing_real = jnp.einsum("tgc,gpc->tgp", feed_rows, bbar_re, precision=lax.Precision.HIGHEST)
    drive_im = jnp.einsum("tgc,gpc->tgp", feed_rows, bbar_im, precision=lax.Precision.HIGHEST)
    old_re = state_real.reshape(seq_count, group_count, state_count)
    old_im = state_imag.reshape(seq_count, group_count, state_count)
    fresh_real = abar_re * old_re - abar_im * old_im + forcing_real
    fresh_imaginary = abar_re * old_im + abar_im * old_re + drive_im
    state_readout = jnp.einsum(
        "ukb,krb->ukr",
        fresh_real,
        output_matrix_real.astype(jnp.float32),
        precision=lax.Precision.HIGHEST,
    ) - jnp.einsum(
        "ukb,krb->ukr",
        fresh_imaginary,
        output_matrix_imaginary.astype(jnp.float32),
        precision=lax.Precision.HIGHEST,
    )
    mixed_rows = state_readout.reshape(
        seq_count, group_count * chan_count
    ) + skip_gain * branch_in.astype(jnp.float32)
    activated = jax.nn.gelu(mixed_rows).astype(jnp.bfloat16)
    return (activated, fresh_real.reshape(seq_count, -1), fresh_imaginary.reshape(seq_count, -1))


def mixer_residual(residual, activated, glu_value, glu_gate, mix_gain):
    value_part = jnp.dot(activated, glu_value, preferred_element_type=jnp.float32)
    gate_part = jnp.dot(activated, glu_gate, preferred_element_type=jnp.float32)
    branch = value_part * jax.nn.sigmoid(gate_part)
    return (residual.astype(jnp.float32) + scaled_norm(branch, mix_gain)).astype(jnp.bfloat16)


def serve_rows(
    residual, branch_in, state_real, state_imag, routes, route_weights, params, capacity
):
    (
        decay_rate,
        frequency,
        log_step,
        input_real,
        input_imag,
        output_matrix_real,
        output_matrix_imaginary,
        skip_gain,
        glu_value,
        glu_gate,
        mix_gain,
        moe_in_gain,
        moe_out_gain,
        expert_gate,
        expert_up,
        expert_down,
        shared_gate,
        shared_up,
        shared_down,
    ) = params
    activated, next_real, next_imag = state_step(
        branch_in,
        state_real,
        state_imag,
        decay_rate,
        frequency,
        log_step,
        input_real,
        input_imag,
        output_matrix_real,
        output_matrix_imaginary,
        skip_gain,
    )
    resid_mid = mixer_residual(residual, activated, glu_value, glu_gate, mix_gain)
    normed = scaled_norm(resid_mid.astype(jnp.float32), moe_in_gain).astype(jnp.bfloat16)
    count = lax.axis_size("ep")
    cap = -(-capacity // ROW_TILE) * ROW_TILE
    planes = residual.shape[0] // cap
    width = count // planes
    layer_out = moe_layer(
        normed,
        resid_mid,
        slot_table(routes, route_weights, planes, width, cap),
        moe_out_gain,
        (expert_gate[0], expert_up[0], expert_down[0]),
        (shared_gate, shared_up, shared_down),
        planes,
        width,
        cap,
    )
    return (layer_out, next_real, next_imag)


def per_device(
    residual,
    branch_in,
    state_real,
    state_imag,
    decay_rate,
    frequency,
    log_step,
    input_real,
    input_imag,
    output_matrix_real,
    output_matrix_imaginary,
    skip_gain,
    glu_value,
    glu_gate,
    mix_gain,
    moe_in_gain,
    moe_out_gain,
    routes,
    route_weights,
    expert_gate,
    expert_up,
    expert_down,
    shared_gate,
    shared_up,
    shared_down,
):
    params = (
        decay_rate,
        frequency,
        log_step,
        input_real,
        input_imag,
        output_matrix_real,
        output_matrix_imaginary,
        skip_gain,
        glu_value,
        glu_gate,
        mix_gain,
        moe_in_gain,
        moe_out_gain,
        expert_gate,
        expert_up,
        expert_down,
        shared_gate,
        shared_up,
        shared_down,
    )
    seq_dev = residual.shape[0]
    capacity = max(2, 4 * seq_dev * routes.shape[1] // (3 * lax.axis_size("ep")))
    return serve_rows(
        residual, branch_in, state_real, state_imag, routes, route_weights, params, capacity
    )


def solution(mesh):
    return jax.shard_map(
        per_device,
        mesh=mesh,
        in_specs=(
            P("ep", None),
            P("ep", None),
            P("ep", None),
            P("ep", None),
            P(),
            P(),
            P(),
            P(),
            P(),
            P(),
            P(),
            P(),
            P(),
            P(),
            P(),
            P(),
            P(),
            P("ep", None),
            P("ep", None),
            P("ep", None, None),
            P("ep", None, None),
            P("ep", None, None),
            P(),
            P(),
            P(),
        ),
        out_specs=(P("ep", None), P("ep", None), P("ep", None)),
        check_vma=False,
    )
```

```python
import functools

import jax
import jax.numpy as jnp
from jax import lax
from jax.experimental import pallas as pl
from jax.experimental.pallas import tpu as pltpu
from jax.sharding import PartitionSpec as P

norm_eps = 1e-06
ROW_TILE = 16
PIECES = 2
MESH = pl.DeviceIdType.MESH


def scaled_norm(row_block, norm_gain):
    return (
        row_block
        * lax.rsqrt(jnp.mean(row_block * row_block, axis=-1, keepdims=True) + norm_eps)
        * norm_gain
    )


def flipped(index, mask):
    out, bit = 0, 1
    while bit <= mask or bit == 1:
        digit = (index // bit) % 2
        out = out + bit * ((digit + 1) % 2 if mask & bit else digit)
        bit *= 2
    return out + (index // bit) * bit


def moe_kernel(
    planes,
    width,
    cap,
    normed,
    resid,
    slot_weights,
    out_gain,
    eg_hbm,
    eu_hbm,
    ed_hbm,
    sg_hbm,
    su_hbm,
    sd_hbm,
    out,
    eg,
    eu,
    ed,
    sg,
    su,
    sd,
    col_rows,
    col_weights,
    x_send,
    x_recv,
    y_send,
    y_recv,
    p_send,
    p_recv,
    total,
    load_sem,
    own_sem,
    row_s,
    row_r,
    wt_s,
    wt_r,
    x_s,
    x_r,
    y_s,
    y_r,
    p_s,
    p_r,
):
    me = lax.axis_index("ep")
    z = me // width
    p = me % width
    model = normed.shape[1]
    chunk = model // PIECES
    columns = [slice(i * chunk, (i + 1) * chunk) for i in range(PIECES)]
    loads = [
        pltpu.make_async_copy(src, dst, load_sem.at[i])
        for i, (src, dst) in enumerate(
            ((sg_hbm, sg), (su_hbm, su), (sd_hbm, sd), (eg_hbm, eg), (eu_hbm, eu), (ed_hbm, ed))
        )
    ]
    for load in loads:
        load.start()

    barrier = pltpu.get_barrier_semaphore()
    for d in range(1, planes):
        pl.semaphore_signal(
            barrier, inc=1, device_id=(flipped(z, d) * width + p,), device_id_type=MESH
        )
    for r in range(1, width):
        pl.semaphore_signal(
            barrier, inc=1, device_id=(z * width + flipped(p, r),), device_id_type=MESH
        )
    pl.semaphore_wait(barrier, planes - 1 + width - 1)

    sends = []

    def send(src, dst, send_sem, recv_sem, target):
        copy = pltpu.make_async_remote_copy(
            src_ref=src,
            dst_ref=dst,
            send_sem=send_sem,
            recv_sem=recv_sem,
            device_id=(target,),
            device_id_type=MESH,
        )
        copy.start()
        sends.append(copy)

    def part(buf, d, q, i):
        return buf.at[d, pl.ds(pl.multiple_of(q * cap, cap), cap), columns[i]]

    for d in range(1, planes):
        zt = flipped(z, d)
        target = zt * width + p
        send(slot_weights.at[zt], col_weights.at[d], wt_s.at[d], wt_r.at[d], target)
        for i in range(PIECES):
            send(
                normed.at[:, columns[i]],
                col_rows.at[d, :, columns[i]],
                row_s.at[d, i],
                row_r.at[d, i],
                target,
            )

    def arrive(buf, sem):
        pltpu.make_async_copy(buf, buf, sem).wait()

    def block_weights(d):
        return slot_weights[z] if d == 0 else col_weights[d]

    def exchange(src, dst, d, i, send_sems, recv_sems, own):
        for r in range(1, width):
            q = flipped(p, r)
            send(
                part(src, d, q, i),
                part(dst, d, p, i),
                send_sems.at[d, r, i],
                recv_sems.at[d, r, i],
                z * width + q,
            )
        pltpu.make_async_copy(part(src, d, p, i), part(dst, d, p, i), own).start()

    def gathered(src, dst, d, i, recv_sems, own):
        for r in range(1, width):
            arrive(part(dst, d, flipped(p, r), i), recv_sems.at[d, r, i])
        pltpu.make_async_copy(part(src, d, p, i), part(dst, d, p, i), own).wait()

    def dispatch(d, i):
        if d:
            if i == 0:
                arrive(col_weights.at[d], wt_r.at[d])
            arrive(col_rows.at[d, :, columns[i]], row_r.at[d, i])
        picks = jnp.where(block_weights(d).T > 0.0, 1.0, 0.0).astype(jnp.bfloat16)
        rows = normed[:, columns[i]] if d == 0 else col_rows[d, :, columns[i]]
        x_send[d, :, columns[i]] = jnp.dot(
            picks, rows, preferred_element_type=jnp.float32
        ).astype(jnp.bfloat16)
        exchange(x_send, x_recv, d, i, x_s, x_r, own_sem.at[0, d, i])

    def hidden(rows, w_gate, w_up):
        gate_part = jnp.dot(rows, w_gate[...], preferred_element_type=jnp.float32)
        up_part = jnp.dot(rows, w_up[...], preferred_element_type=jnp.float32)
        return (jax.nn.silu(gate_part) * up_part).astype(jnp.bfloat16)

    def expert(d):
        for i in range(PIECES):
            gathered(x_send, x_recv, d, i, x_r, own_sem.at[0, d, i])
        if d == 0:
            for load in loads[3:]:
                load.wait()
        mid = hidden(x_recv[d], eg, eu)
        for i in range(PIECES):
            y_send[d, :, columns[i]] = jnp.dot(
                mid, ed[:, columns[i]], preferred_element_type=jnp.float32
            ).astype(jnp.bfloat16)
            exchange(y_send, y_recv, d, i, y_s, y_r, own_sem.at[1, d, i])

    def combine(d):
        weights = block_weights(d)
        high = weights.astype(jnp.bfloat16)
        low = (weights - high.astype(jnp.float32)).astype(jnp.bfloat16)
        for i in range(PIECES):
            gathered(y_send, y_recv, d, i, y_r, own_sem.at[1, d, i])
            rows = y_recv[d, :, columns[i]]
            partial = jnp.dot(high, rows, preferred_element_type=jnp.float32) + jnp.dot(
                low, rows, preferred_element_type=jnp.float32
            )
            if d == 0:
                total[:, columns[i]] += partial
            else:
                p_send[d, :, columns[i]] = partial.astype(jnp.bfloat16)
                send(
                    p_send.at[d, :, columns[i]],
                    p_recv.at[d, :, columns[i]],
                    p_s.at[d, i],
                    p_r.at[d, i],
                    flipped(z, d) * width + p,
                )

    for i in range(PIECES):
        dispatch(0, i)
    for load in loads[:3]:
        load.wait()
    mid = hidden(normed[...], sg, su)
    for i in range(PIECES):
        total[:, columns[i]] = jnp.dot(
            mid, sd[:, columns[i]], preferred_element_type=jnp.float32
        )
    last = planes - 1
    for d in range(1, planes):
        for i in range(PIECES):
            dispatch(d, i)
            if i == 0 and d > 1 and d < last:
                expert(d - 1)
        if d == 1:
            expert(0)
    if last > 1:
        expert(last - 1)
    for d in range(1, last - 1):
        combine(d)
    if last > 0:
        expert(last)
    if last > 1:
        combine(last - 1)
    combine(0)
    if last > 0:
        combine(last)
    for d in range(1, planes):
        for i in range(PIECES):
            arrive(p_recv.at[d, :, columns[i]], p_r.at[d, i])
    combined = total[...]
    for d in range(1, planes):
        combined = combined + p_recv[d].astype(jnp.float32)
    out[...] = (
        resid[...].astype(jnp.float32) + scaled_norm(combined, out_gain[...])
    ).astype(out.dtype)
    for copy in sends:
        copy.wait_send()


def moe_layer(
    normed, resid_mid, slot_weights, moe_out_gain, experts, shared_weights, planes, width, cap
):
    seq_count, model = normed.shape
    half = jnp.bfloat16
    vmem = pl.BlockSpec(memory_space=pltpu.VMEM)
    hbm = pl.BlockSpec(memory_space=pl.ANY)
    slots = (planes, width * cap, model)
    dense = (planes, seq_count, model)
    dma = pltpu.SemaphoreType.DMA
    weights = (*experts, *shared_weights)
    return pl.pallas_call(
        functools.partial(moe_kernel, planes, width, cap),
        out_shape=jax.ShapeDtypeStruct((seq_count, model), half),
        in_specs=[vmem] * 4 + [hbm] * 6,
        out_specs=vmem,
        scratch_shapes=[pltpu.VMEM(w.shape, w.dtype) for w in weights]
        + [
            pltpu.VMEM(dense, half),
            pltpu.VMEM(slot_weights.shape, jnp.float32),
            pltpu.VMEM(slots, half),
            pltpu.VMEM(slots, half),
            pltpu.VMEM(slots, half),
            pltpu.VMEM(slots, half),
            pltpu.VMEM(dense, half),
            pltpu.VMEM(dense, half),
            pltpu.VMEM((seq_count, model), jnp.float32),
            dma((6,)),
            dma((2, planes, PIECES)),
            dma((planes, PIECES)),
            dma((planes, PIECES)),
            dma((planes,)),
            dma((planes,)),
            *[dma((planes, width, PIECES))] * 4,
            dma((planes, PIECES)),
            dma((planes, PIECES)),
        ],
        compiler_params=pltpu.CompilerParams(
            collective_id=0, has_side_effects=True, vmem_limit_bytes=60 * 1024 * 1024
        ),
        name="moe_exchange",
    )(normed, resid_mid, slot_weights, moe_out_gain[None, :], *weights)


def slot_table(routes, route_weights, planes, width, cap):
    seq_count, top_count = routes.shape
    columns = planes * width * cap
    column = jnp.arange(columns, dtype=jnp.int32)
    column_expert = (column // cap).reshape(planes, 1, width * cap)
    column_slot = (column % cap).reshape(planes, 1, width * cap)
    match = routes.T[:, None, :, None] == column_expert[None]
    chosen = jnp.any(match, axis=0)
    weight = jnp.sum(jnp.where(match, route_weights.T[:, None, :, None], 0.0), axis=0)
    earlier = jnp.tril(jnp.ones((seq_count, seq_count), jnp.bfloat16), -1)
    rank = jnp.einsum(
        "ut,ztj->zuj", earlier, chosen.astype(jnp.bfloat16), preferred_element_type=jnp.float32
    )
    return jnp.where(chosen & (rank == column_slot.astype(jnp.float32)), weight, 0.0)


def wide(block, groups):
    rows, states = block.shape
    tiled = jnp.concatenate([block] * groups, axis=1)
    shape = (rows, groups * states)
    row = lax.broadcasted_iota(jnp.int32, shape, 0) // (rows // groups)
    column = lax.broadcasted_iota(jnp.int32, shape, 1) // states
    return jnp.where(row == column, tiled, 0.0)


def halves(value):
    high = value.astype(jnp.bfloat16)
    return high, (value - high.astype(jnp.float32)).astype(jnp.bfloat16)


def mixer_kernel(
    groups,
    residual,
    feed,
    state_re,
    state_im,
    abar_re,
    abar_im,
    bbar_re,
    bbar_im,
    out_re,
    out_im,
    skip,
    value_hbm,
    gate_hbm,
    mix_gain,
    in_gain,
    resid_mid,
    normed,
    next_re,
    next_im,
    old_re,
    old_im,
    new_re,
    new_im,
    value,
    gate,
    active,
    in_sem,
    out_sem,
    glu_sem,
):
    states = abar_re.shape[1]
    chans = bbar_re.shape[0] // abar_re.shape[0]
    lanes = groups * states
    feeds = groups * chans
    count = abar_re.shape[0] // groups

    def piece(n):
        return slice(n * lanes, (n + 1) * lanes)

    def read(n):
        return [
            pltpu.make_async_copy(src.at[:, piece(n)], dst.at[:, piece(n)], in_sem.at[k, n])
            for k, (src, dst) in enumerate(((state_re, old_re), (state_im, old_im)))
        ]

    def write(n):
        return [
            pltpu.make_async_copy(src.at[:, piece(n)], dst.at[:, piece(n)], out_sem.at[k, n])
            for k, (src, dst) in enumerate(((new_re, next_re), (new_im, next_im)))
        ]

    glu = [
        pltpu.make_async_copy(value_hbm, value, glu_sem.at[0]),
        pltpu.make_async_copy(gate_hbm, gate, glu_sem.at[1]),
    ]
    for n in range(count):
        for copy in read(n):
            copy.start()
    for copy in glu:
        copy.start()

    nt = (((1,), (1,)), ((), ()))
    for n in range(count):
        rows = slice(n * feeds, (n + 1) * feeds)
        some = slice(n * groups, (n + 1) * groups)
        u = feed[:, rows]
        a_re = jnp.sum(wide(abar_re[some, :], groups), axis=0, keepdims=True)
        a_im = jnp.sum(wide(abar_im[some, :], groups), axis=0, keepdims=True)

        def force(bbar):
            high, low = halves(wide(bbar[rows, :], groups))
            return jnp.dot(u, high, preferred_element_type=jnp.float32) + jnp.dot(
                u, low, preferred_element_type=jnp.float32
            )

        def readout(fresh, matrix):
            weights = wide(matrix[rows, :].astype(jnp.float32), groups).astype(jnp.bfloat16)
            high, low = halves(fresh)
            return lax.dot_general(
                high, weights, nt, preferred_element_type=jnp.float32
            ) + lax.dot_general(low, weights, nt, preferred_element_type=jnp.float32)

        for copy in read(n):
            copy.wait()
        was_re, was_im = old_re[:, piece(n)], old_im[:, piece(n)]
        fresh_re = a_re * was_re - a_im * was_im + force(bbar_re)
        fresh_im = a_re * was_im + a_im * was_re + force(bbar_im)
        new_re[:, piece(n)] = fresh_re
        new_im[:, piece(n)] = fresh_im
        for copy in write(n):
            copy.start()
        mixed = (
            readout(fresh_re, out_re)
            - readout(fresh_im, out_im)
            + skip[:, rows] * u.astype(jnp.float32)
        )
        active[:, rows] = jax.nn.gelu(mixed).astype(jnp.bfloat16)
    for copy in glu:
        copy.wait()
    acts = active[...]
    value_part = jnp.dot(acts, value[...], preferred_element_type=jnp.float32)
    gate_part = jnp.dot(acts, gate[...], preferred_element_type=jnp.float32)
    branch = value_part * jax.nn.sigmoid(gate_part)
    mid = (residual[...].astype(jnp.float32) + scaled_norm(branch, mix_gain[...])).astype(
        jnp.bfloat16
    )
    resid_mid[...] = mid
    normed[...] = scaled_norm(mid.astype(jnp.float32), in_gain[...]).astype(jnp.bfloat16)
    for n in range(count):
        for copy in write(n):
            copy.wait()


def mixer(
    residual,
    branch_in,
    state_real,
    state_imag,
    decay_rate,
    frequency,
    log_step,
    input_real,
    input_imag,
    output_matrix_real,
    output_matrix_imaginary,
    skip_gain,
    glu_value,
    glu_gate,
    mix_gain,
    moe_in_gain,
):
    group_count, state_count = decay_rate.shape
    step_size = jnp.exp(log_step)[:, None]
    magnitude = jnp.exp(-decay_rate * step_size)
    abar_re = magnitude * jnp.cos(frequency * step_size)
    abar_im = magnitude * jnp.sin(frequency * step_size)
    lam_re = -decay_rate
    denominator = lam_re * lam_re + frequency * frequency
    numer_re = abar_re - 1.0
    coef_re = ((numer_re * lam_re + abar_im * frequency) / denominator)[:, None, :]
    coef_im = ((abar_im * lam_re - numer_re * frequency) / denominator)[:, None, :]
    b_real = input_real.astype(jnp.float32).transpose(0, 2, 1)
    b_imag = input_imag.astype(jnp.float32).transpose(0, 2, 1)
    bbar_re = (coef_re * b_real - coef_im * b_imag).reshape(-1, state_count)
    bbar_im = (coef_re * b_imag + coef_im * b_real).reshape(-1, state_count)
    groups = max(1, 128 // input_real.shape[2])
    count = group_count // groups
    vmem = pl.BlockSpec(memory_space=pltpu.VMEM)
    hbm = pl.BlockSpec(memory_space=pl.ANY)
    state = state_real.shape
    rows = jax.ShapeDtypeStruct(residual.shape, jnp.bfloat16)
    dma = pltpu.SemaphoreType.DMA
    return pl.pallas_call(
        functools.partial(mixer_kernel, groups),
        out_shape=(
            rows,
            rows,
            jax.ShapeDtypeStruct(state, jnp.float32),
            jax.ShapeDtypeStruct(state, jnp.float32),
        ),
        in_specs=[vmem, vmem, hbm, hbm] + [vmem] * 7 + [hbm, hbm, vmem, vmem],
        out_specs=(vmem, vmem, hbm, hbm),
        scratch_shapes=[
            *[pltpu.VMEM(state, jnp.float32)] * 4,
            pltpu.VMEM(glu_value.shape, jnp.bfloat16),
            pltpu.VMEM(glu_gate.shape, jnp.bfloat16),
            pltpu.VMEM(branch_in.shape, jnp.bfloat16),
            dma((2, count)),
            dma((2, count)),
            dma((2,)),
        ],
        compiler_params=pltpu.CompilerParams(vmem_limit_bytes=60 * 1024 * 1024),
        name="mixer",
    )(
        residual,
        branch_in,
        state_real,
        state_imag,
        abar_re,
        abar_im,
        bbar_re,
        bbar_im,
        output_matrix_real.reshape(-1, state_count),
        output_matrix_imaginary.reshape(-1, state_count),
        skip_gain[None, :],
        glu_value,
        glu_gate,
        mix_gain[None, :],
        moe_in_gain[None, :],
    )


def serve_rows(
    residual, branch_in, state_real, state_imag, routes, route_weights, params, capacity
):
    (
        decay_rate,
        frequency,
        log_step,
        input_real,
        input_imag,
        output_matrix_real,
        output_matrix_imaginary,
        skip_gain,
        glu_value,
        glu_gate,
        mix_gain,
        moe_in_gain,
        moe_out_gain,
        expert_gate,
        expert_up,
        expert_down,
        shared_gate,
        shared_up,
        shared_down,
    ) = params
    resid_mid, normed, next_real, next_imag = mixer(
        residual,
        branch_in,
        state_real,
        state_imag,
        decay_rate,
        frequency,
        log_step,
        input_real,
        input_imag,
        output_matrix_real,
        output_matrix_imaginary,
        skip_gain,
        glu_value,
        glu_gate,
        mix_gain,
        moe_in_gain,
    )
    count = lax.axis_size("ep")
    cap = -(-capacity // ROW_TILE) * ROW_TILE
    planes = residual.shape[0] // cap
    width = count // planes
    layer_out = moe_layer(
        normed,
        resid_mid,
        slot_table(routes, route_weights, planes, width, cap),
        moe_out_gain,
        (expert_gate[0], expert_up[0], expert_down[0]),
        (shared_gate, shared_up, shared_down),
        planes,
        width,
        cap,
    )
    return (layer_out, next_real, next_imag)


def per_device(
    residual,
    branch_in,
    state_real,
    state_imag,
    decay_rate,
    frequency,
    log_step,
    input_real,
    input_imag,
    output_matrix_real,
    output_matrix_imaginary,
    skip_gain,
    glu_value,
    glu_gate,
    mix_gain,
    moe_in_gain,
    moe_out_gain,
    routes,
    route_weights,
    expert_gate,
    expert_up,
    expert_down,
    shared_gate,
    shared_up,
    shared_down,
):
    params = (
        decay_rate,
        frequency,
        log_step,
        input_real,
        input_imag,
        output_matrix_real,
        output_matrix_imaginary,
        skip_gain,
        glu_value,
        glu_gate,
        mix_gain,
        moe_in_gain,
        moe_out_gain,
        expert_gate,
        expert_up,
        expert_down,
        shared_gate,
        shared_up,
        shared_down,
    )
    seq_dev = residual.shape[0]
    capacity = max(2, 4 * seq_dev * routes.shape[1] // (3 * lax.axis_size("ep")))
    return serve_rows(
        residual, branch_in, state_real, state_imag, routes, route_weights, params, capacity
    )


def solution(mesh):
    return jax.shard_map(
        per_device,
        mesh=mesh,
        in_specs=(
            P("ep", None),
            P("ep", None),
            P("ep", None),
            P("ep", None),
            P(),
            P(),
            P(),
            P(),
            P(),
            P(),
            P(),
            P(),
            P(),
            P(),
            P(),
            P(),
            P(),
            P("ep", None),
            P("ep", None),
            P("ep", None, None),
            P("ep", None, None),
            P("ep", None, None),
            P(),
            P(),
            P(),
        ),
        out_specs=(P("ep", None), P("ep", None), P("ep", None)),
        check_vma=False,
    )
```
